32 devices in a mesh: grp: 2 (over x), sp: 4 (over y, core), tp: 4 (over z).
Axes of the slice: x: 2, y: 2, z: 4, core: 2. Of those that a mesh axis runs over, the one named last changes fastest.
Arguments:
- layer_input: bfloat16 [8, 1024, 2048], P(('grp', 'tp'), 'sp'), parts along dimension 0, may hold values from -6 to 6
- norm_gain: bfloat16 [2048], replicated, may hold values from 0.099609375 to 1.8984375
- key_weight: bfloat16 [2048, 1024], replicated, may hold values from -0.125 to 0.125
- value_weight: bfloat16 [2048, 1024], replicated, may hold values from -0.125 to 0.125
- input_gate_weight: bfloat16 [2048, 8], replicated, may hold values from -0.125 to 0.125
- forget_gate_weight: bfloat16 [2048, 8], replicated, may hold values from -0.125 to 0.125
- conv_weight: float32 [4, 1024], replicated, may hold values from -3 to 3
- input_shift: float32 [8, 8, 1024], P(('grp', 'sp'), 'tp'), parts along dimension 0, may hold values from -4 to 302
- forget_shift: float32 [8, 8, 1024], P(('grp', 'sp'), 'tp'), parts along dimension 0, may hold values from 0 to 10.1
- new_query: bfloat16 [8, 8, 128], P(('grp', 'sp'), 'tp'), parts along dimension 0, may hold values from 0.1 to 2
- new_key: bfloat16 [8, 8, 128], P(('grp', 'sp'), 'tp'), parts along dimension 0, may hold values from -6 to 6
- new_value: bfloat16 [8, 8, 128], P(('grp', 'sp'), 'tp'), parts along dimension 0, may hold values from -6 to 6
- new_input: float32 [8, 8], P(('grp', 'sp'), 'tp'), parts along dimension 0, may hold values from 2 to 6
- new_forget: float32 [8, 8], P(('grp', 'sp'), 'tp'), parts along dimension 0, may hold values from -1 to 3
Outputs:
- key_cache: bfloat16 [8, 8, 1024, 128], P(('grp', 'sp'), 'tp'), parts along dimension 0
- value_cache: bfloat16 [8, 8, 1024, 128], P(('grp', 'sp'), 'tp'), parts along dimension 0
- weight_cache: float32 [8, 8, 1024], P(('grp', 'sp'), 'tp'), parts along dimension 0
- first_read: bfloat16 [8, 8, 128], P(('grp', 'sp'), 'tp'), parts along dimension 0
The draws below stay inside these ranges and needn't reach their ends.
There are 2 independent parts, one for each index of `grp`. The reference program is written for one: setup_inputs(seed, part) draws one part's arguments, and reference() takes and returns one part's arrays. A program takes and returns all parts, laid end to end along the dimension named above; an argument that names none is the same for every part. Nothing has to cross between parts.
All inputs are finite; a program needn't handle non-finite values.
Results may differ from the reference program's by a relative error of at most 0.012.
Values may be sent and summed in bfloat16 or wider, within the bound.
A program may use at most 64 MiB of HBM per device.

```python
import jax
import jax.numpy as jnp
from jax import lax

D = 2048
HEADS = 8
DK = 128
CONV = 4
POS_DEV = 256
SEQS = 4
LENGTH = 1024


def draw_input_shift(key, part):
    subkeys = jax.random.split(key, 1)
    return jnp.clip(jax.random.normal(subkeys[0], (SEQS, HEADS, LENGTH), jnp.float32), -4.0, 4.0)


def draw_forget_shift(key, part):
    subkeys = jax.random.split(key, 5)
    slow_share = 0.5
    slower = jax.random.uniform(subkeys[0], (SEQS, HEADS, 1), jnp.float32) < slow_share
    slow_level = jnp.log(jnp.float32(LENGTH))
    fast_level = jax.random.uniform(subkeys[1], (SEQS, HEADS, 1), jnp.float32, 3.4, 4.6)
    block_list = LENGTH // POS_DEV
    factor = jax.random.uniform(subkeys[2], (SEQS, HEADS, block_list, 1), jnp.float32, -0.7, 0.7)
    factor = jnp.broadcast_to(factor, (SEQS, HEADS, block_list, POS_DEV)).reshape(SEQS, HEADS, LENGTH)
    level_values = jnp.where(slower, slow_level, fast_level) + factor
    targets = jax.random.randint(subkeys[3], (SEQS, HEADS, 4), 0, LENGTH)
    level_heights = jax.random.uniform(subkeys[4], (SEQS, HEADS, 4), jnp.float32, 0.0, 1.4)
    places = jnp.arange(LENGTH)
    match_hits = places[None, None, None, :] == targets[:, :, :, None]
    surge_counts = jnp.any(match_hits, axis=2)
    surge_level = jnp.max(jnp.where(match_hits, level_heights[:, :, :, None], -1.0), axis=2)
    return jnp.where(surge_counts, surge_level, level_values)


def draw_new_query(key, part):
    subkeys = jax.random.split(jax.random.fold_in(key, 17), 2)
    drawn = 1.0 + 0.5 * jax.random.normal(subkeys[1], (SEQS, HEADS, DK), jnp.float32)
    return jnp.clip(drawn, 0.1, 2.0).astype(jnp.bfloat16)


def shard_levels(own_key, extent, cuts, least, high):
    level, own = 1.0, jax.random.fold_in(own_key, 6)
    for axis_at, blocks in cuts:
        heights = jnp.exp(jax.random.uniform(jax.random.fold_in(own, axis_at), (blocks,), jnp.float32, least / len(cuts), high / len(cuts)))
        level = level * jnp.repeat(heights, extent[axis_at] // blocks).reshape([-1 if axis == axis_at else 1 for axis in range(len(extent))])
    return level


def bell_draw(own_key, extent, deviation, bound, pieces=(), held_as=jnp.bfloat16):
    values = jax.random.normal(own_key, extent, jnp.float32) * deviation
    if len(pieces) > 0:
        values = shard_levels(own_key, extent, pieces, -0.22, 0.18) * values
    return jnp.clip(values, min=-bound, max=bound).astype(held_as)


def setup_inputs(seed: int = 0, part: int = 0) -> dict:
    key_list = jax.random.split(jax.random.key(seed), 15)
    part_keys = jax.random.split(jax.random.fold_in(key_list[14], part), 15)
    return {
        "layer_input": bell_draw(part_keys[0], (SEQS, LENGTH, D), 1.0, 6.0, ((0, 4), (1, 4))),
        "norm_gain": jnp.clip(1.0 + 0.18 * jax.random.normal(key_list[1], (D,), jnp.float32), 0.099609375, 1.8984375).astype(jnp.bfloat16),
        "key_weight": bell_draw(key_list[2], (D, HEADS * DK), D ** -0.5, 0.125),
        "value_weight": bell_draw(key_list[3], (D, HEADS * DK), D ** -0.5, 0.125),
        "input_gate_weight": bell_draw(key_list[4], (D, HEADS), D ** -0.5, 0.125),
        "forget_gate_weight": bell_draw(key_list[5], (D, HEADS), D ** -0.5, 0.125),
        "conv_weight": bell_draw(key_list[6], (CONV, HEADS * DK), 0.5, 3.0, (), jnp.float32),
        "input_shift": draw_input_shift(jax.random.fold_in(jax.random.fold_in(key_list[14], part), 71), part),
        "forget_shift": draw_forget_shift(jax.random.fold_in(jax.random.fold_in(key_list[14], part), 71), part),
        "new_query": draw_new_query(jax.random.fold_in(jax.random.fold_in(key_list[14], part), 71), part),
        "new_key": bell_draw(part_keys[10], (SEQS, HEADS, DK), 1.0, 6.0, ((0, 4), (1, 4))),
        "new_value": bell_draw(part_keys[11], (SEQS, HEADS, DK), 1.0, 6.0, ((0, 4), (1, 4))),
        "new_input": jnp.clip(2.0 + 4.0 * jax.random.uniform(part_keys[12], (SEQS, HEADS), jnp.float32) ** shard_levels(part_keys[12], (SEQS, HEADS), ((0, 4), (1, 4)), -0.2, 0.2), 2.0, 6.0),
        "new_forget": jnp.clip(-1.0 + 4.0 * jax.random.uniform(part_keys[13], (SEQS, HEADS), jnp.float32) ** shard_levels(part_keys[13], (SEQS, HEADS), ((0, 4), (1, 4)), -0.2, 0.2), -1.0, 3.0),
    }


epsilon = 1e-06

def one_sequence(token_rows, norm_gain, key_weight, value_weight, input_gate_weight, forget_gate_weight, conv_weight):
    widened = token_rows.astype(jnp.float32)
    normed = (widened * lax.rsqrt(lax.optimization_barrier(jnp.mean(widened * widened, axis=-1, keepdims=True)) + epsilon) * norm_gain.astype(jnp.float32)).astype(jnp.bfloat16)
    key_linear = jnp.dot(normed, key_weight, preferred_element_type=jnp.float32).astype(jnp.bfloat16)
    values = jnp.dot(normed, value_weight, preferred_element_type=jnp.float32).astype(jnp.bfloat16)
    input_linear = jnp.dot(normed, input_gate_weight, preferred_element_type=jnp.float32).astype(jnp.bfloat16)
    forget_linear = jnp.dot(normed, forget_gate_weight, preferred_element_type=jnp.float32).astype(jnp.bfloat16)
    padded = jnp.pad(key_linear.astype(jnp.float32), ((CONV - 1, 0), (0, 0)))
    summed = padded[0:LENGTH] * conv_weight[0]
    for offset in range(1, CONV):
        summed = summed + padded[offset:offset + LENGTH] * conv_weight[offset]
    keys = jax.nn.silu(summed).astype(jnp.bfloat16)
    keys = keys.reshape(LENGTH, HEADS, DK).transpose(1, 0, 2)
    values = values.reshape(LENGTH, HEADS, DK).transpose(1, 0, 2)
    return (keys, values, input_linear.T, forget_linear.T)

def read_cache(keys, values, input_linear, forget_linear, input_shift, forget_shift, new_query, new_key, new_value, new_input, new_forget):
    scaling = DK ** (-0.5)
    log_forget = jax.nn.log_sigmoid(forget_linear.astype(jnp.float32) + forget_shift)
    suffix = lax.cumsum(log_forget, axis=2, reverse=True) - log_forget
    new_decay = jax.nn.log_sigmoid(new_forget)
    log_weight = input_linear.astype(jnp.float32) + input_shift + suffix + new_decay[:, :, None]
    largest = jnp.maximum(lax.optimization_barrier(jnp.max(log_weight, axis=2)), new_input)
    weight_cache = jnp.exp(log_weight - largest[:, :, None])
    new_weight = jnp.exp(new_input - largest)
    matched = jnp.einsum('bhlk,bhk->bhl', keys.astype(jnp.float32), new_query.astype(jnp.float32))
    scores = (weight_cache * matched * scaling).astype(jnp.bfloat16)
    fresh_match = lax.optimization_barrier(jnp.sum(new_key.astype(jnp.float32) * new_query.astype(jnp.float32), axis=2))
    new_score = (new_weight * fresh_match * scaling).astype(jnp.bfloat16)
    denominator = lax.optimization_barrier(jnp.sum(scores.astype(jnp.float32), axis=2)) + new_score.astype(jnp.float32)
    numerator = jnp.einsum('bhl,bhlk->bhk', scores.astype(jnp.float32), values.astype(jnp.float32))
    numerator = numerator + new_score.astype(jnp.float32)[:, :, None] * new_value.astype(jnp.float32)
    first_read = (numerator / jnp.maximum(jnp.abs(denominator), 1.0)[:, :, None]).astype(jnp.bfloat16)
    return (weight_cache, first_read)

def reference(layer_input, norm_gain, key_weight, value_weight, input_gate_weight, forget_gate_weight, conv_weight, input_shift, forget_shift, new_query, new_key, new_value, new_input, new_forget):

    def project(token_rows):
        return one_sequence(token_rows, norm_gain, key_weight, value_weight, input_gate_weight, forget_gate_weight, conv_weight)
    keys, values, input_linear, forget_linear = lax.map(project, layer_input)
    weight_cache, first_read = read_cache(keys, values, input_linear, forget_linear, input_shift, forget_shift, new_query, new_key, new_value, new_input, new_forget)
    return (keys, values, weight_cache, first_read)
```

```python
import functools

import jax
import jax.numpy as jnp
from jax import lax
from jax.experimental import pallas as pl
from jax.experimental.pallas import tpu as pltpu
from jax.sharding import PartitionSpec as P

MESH = pl.DeviceIdType.MESH
epsilon = 1e-06
SPLIT = 2


def log_sigmoid(x):
    return jnp.minimum(x, 0.0) - jnp.log1p(jnp.exp(-jnp.abs(x)))


def kernel(
    dims,
    x_ref,
    gain_ref,
    wi_ref,
    wf_ref,
    conv_ref,
    ishift_ref,
    fshift_ref,
    query_ref,
    nkey_ref,
    nvalue_ref,
    ninput_ref,
    nforget_ref,
    wk_ref,
    wv_ref,
    keys_out,
    values_out,
    weight_out,
    read_out,
    wbuf,
    normed,
    comp,
    relay,
    final,
    gcomp,
    grelay,
    gfinal,
    ext,
    kconv,
    w_sem,
    s1_send,
    s1_recv,
    s2_send,
    f_recv,
    o_sem,
):
    n, nsp, ns, nd, pos, heads, hl, dk, taps = dims
    chunks = [(kv, r) for kv in range(2) for r in range(SPLIT)]
    C = len(chunks)
    rows = pos // SPLIT
    length = nsp * pos
    t = lax.axis_index("tp")
    p = lax.axis_index("sp")
    high = (2 * t) // n
    direction = 1 - 2 * high
    targets = [lax.rem(t + direction * (1 + k) + n, n) for k in range(n)]

    barrier = pltpu.get_barrier_semaphore()
    for k in range(n - 1):
        pl.semaphore_signal(barrier, inc=1, device_id={"tp": targets[k]}, device_id_type=MESH)
    for k in range(nsp - 1):
        pl.semaphore_signal(
            barrier, inc=1, device_id={"sp": lax.rem(p + 1 + k, nsp)}, device_id_type=MESH
        )

    def weight_copy(k, kv):
        columns = pl.ds(pl.multiple_of(targets[k] * (hl * dk), dk), hl * dk)
        source = wv_ref if kv else wk_ref
        return pltpu.make_async_copy(source.at[:, columns], wbuf.at[k, kv], w_sem.at[k, kv])

    for k in range(n):
        for kv in range(2):
            weight_copy(k, kv).start()

    gain = gain_ref[...].astype(jnp.float32)
    step = 32
    for i in range(ns):

        @pl.loop(0, pos // step)
        def _(at):
            window = pl.ds(pl.multiple_of(at * step, step), step)
            wide = x_ref[i, window, :].astype(jnp.float32)
            mean = jnp.mean(wide * wide, axis=-1, keepdims=True)
            normed[i, window, :] = (wide * lax.rsqrt(mean + epsilon) * gain).astype(jnp.bfloat16)

    for i in range(ns):
        for at, w in enumerate((wi_ref, wf_ref)):
            g = lax.dot_general(
                w[...], normed[i], (((0,), (1,)), ((), ())), preferred_element_type=jnp.float32
            )
            gcomp[i, at * heads : (at + 1) * heads, :] = g.astype(jnp.bfloat16)

    def part(buf, lead, c):
        kv, r = chunks[c]
        return buf.at[(*lead, kv, slice(None), pl.ds(r * rows, rows), slice(None))]

    def s1_source(k, i, c):
        return gcomp.at[i] if c == C else part(comp, (k, i), c)

    def s1_target(b, i, c):
        return grelay.at[b, i] if c == C else part(relay, (b, i), c)

    def s1_copy(k, i, c):
        return pltpu.make_async_remote_copy(
            src_ref=s1_source(k, i, c),
            dst_ref=s1_target(t, i, c),
            send_sem=s1_send.at[k, i, c],
            recv_sem=s1_recv.at[t, i, c],
            device_id={"tp": targets[k]},
            device_id_type=MESH,
        )

    def f_target(d, at, c):
        if c == C:
            return gfinal.at[d, at]
        kv, r = chunks[c]
        window = pl.ds(pl.multiple_of(at * pos + r * rows, rows), rows)
        return final.at[d, kv, :, window, :]

    def forward(k, b, i, c, begin):
        s = b * ns + i
        q = s // nd
        d = lax.rem(s, nd)
        source = s1_source(n - 1, i, c) if k == n - 1 else s1_target(b, i, c)
        remote = pltpu.make_async_remote_copy(
            src_ref=source,
            dst_ref=f_target(d, p, c),
            send_sem=s2_send.at[k, i, c],
            recv_sem=f_recv.at[d, p, c],
            device_id={"sp": q},
            device_id_type=MESH,
        )

        @pl.when(q != p)
        def _():
            if begin:
                remote.start()
            else:
                remote.wait_send()

        if begin:

            @pl.when(q == p)
            def _():
                pltpu.make_async_copy(source, f_target(d, p, c), f_recv.at[d, p, c]).start()

    def compute(k):
        for kv in range(2):
            weight_copy(k, kv).wait()
            for i in range(ns):
                y = jnp.dot(normed[i], wbuf[k, kv], preferred_element_type=jnp.float32)
                for h in range(hl):
                    comp[k, i, kv, h] = y[:, h * dk : (h + 1) * dk].astype(jnp.bfloat16)
            if k == 0 and kv == 0:
                pl.semaphore_wait(barrier, n - 1 + nsp - 1)
                for i in range(ns):
                    for to in range(n - 1):
                        s1_copy(to, i, C).start()
                    forward(n - 1, t, i, C, True)
            for i in range(ns):
                for c in range(C):
                    if chunks[c][0] == kv:
                        if k == n - 1:
                            forward(k, t, i, c, True)
                        else:
                            s1_copy(k, i, c).start()

    for k in range(n):
        compute(k)

    def origin(k):
        lower = k + (k >= t).astype(jnp.int32)
        upper = n - 1 - (k + (k >= n - 1 - t).astype(jnp.int32))
        return jnp.where(high == 0, lower, upper)

    def relay_step(k, c):
        b = origin(k)
        for i in range(ns):
            place = s1_target(b, i, c)
            pltpu.make_async_copy(place, place, s1_recv.at[b, i, c]).wait()
            forward(k, b, i, c, True)

    for k in range(n - 1):
        relay_step(k, C)
    for k in range(n - 1):
        for c in range(C):
            relay_step(k, c)

    def arrived(d, at, c):
        place = f_target(d, at, c)
        pltpu.make_async_copy(place, place, f_recv.at[d, at, c]).wait()

    scaling = dk ** (-0.5)
    lane = lax.broadcasted_iota(jnp.int32, (8, length), 1)
    row = lax.broadcasted_iota(jnp.int32, (2 * heads, pos), 0)
    weights, fresh = {}, {}
    for d in range(nd):
        for at in range(nsp):
            arrived(d, at, C)
        for h in range(hl):

            def gate(base):
                pieces = [
                    jnp.sum(
                        jnp.where(
                            row == base + t * hl + h, gfinal[d, at].astype(jnp.float32), 0.0
                        ),
                        axis=0,
                        keepdims=True,
                    )
                    for at in range(nsp)
                ]
                return jnp.concatenate(pieces, axis=1)

            log_forget = log_sigmoid(gate(heads) + fshift_ref[d, h : h + 1, :])
            suffix = pltpu.roll(jnp.broadcast_to(log_forget, (8, length)), length - 1, 1)
            suffix = jnp.where(lane < length - 1, suffix, 0.0)
            hop = 1
            while hop < length:
                moved = pltpu.roll(suffix, length - hop, 1)
                suffix = suffix + jnp.where(lane < length - hop, moved, 0.0)
                hop *= 2
            new_input = ninput_ref[d : d + 1, h : h + 1]
            decay = log_sigmoid(nforget_ref[d : d + 1, h : h + 1])
            log_weight = gate(0) + ishift_ref[d, h : h + 1, :] + suffix + decay
            largest = jnp.maximum(jnp.max(log_weight, axis=1, keepdims=True), new_input)
            weight = jnp.exp(log_weight - largest)
            weight_out[d, h : h + 1, :] = weight[0:1]
            query = query_ref[d, h : h + 1, :].astype(jnp.float32)
            match = jnp.sum(
                nkey_ref[d, h : h + 1, :].astype(jnp.float32) * query, axis=1, keepdims=True
            )
            score = jnp.exp(new_input - largest) * match * scaling
            fresh[d, h] = score.astype(jnp.bfloat16).astype(jnp.float32)
            weights[d, h] = weight

    def key_copy(d, at):
        window = pl.ds(at * pos, pos)
        return pltpu.make_async_copy(
            kconv.at[d, :, window, :], keys_out.at[d, :, window, :], o_sem.at[d, at, C]
        )

    def value_copy(d, at, c):
        r = chunks[c][1]
        window = pl.ds(at * pos + r * rows, rows)
        return pltpu.make_async_copy(
            final.at[d, 1, :, window, :], values_out.at[d, :, window, :], o_sem.at[d, at, c]
        )

    for d in range(nd):
        ext[:, 0:8, :] = jnp.zeros((hl, 8, dk), jnp.float32)
        for at in range(nsp):
            for c in range(C):
                if chunks[c][0] == 0:
                    arrived(d, at, c)
            for h in range(hl):
                ext[h, 8 + at * pos : 8 + (at + 1) * pos, :] = final[
                    d, 0, h, at * pos : (at + 1) * pos, :
                ].astype(jnp.float32)
                tap = conv_ref[
                    :, pl.ds(pl.multiple_of((t * hl + h) * dk, dk), dk)
                ]
                summed = None
                for o in range(taps):
                    start = 8 - (taps - 1) + o + at * pos
                    term = ext[h, start : start + pos, :] * tap[o : o + 1, :]
                    summed = term if summed is None else summed + term
                kconv[d, h, at * pos : (at + 1) * pos, :] = jax.nn.silu(summed).astype(
                    jnp.bfloat16
                )
            key_copy(d, at).start()
        scores = []
        for h in range(hl):
            query = jnp.broadcast_to(query_ref[d, h : h + 1, :], (8, dk))
            matched = lax.dot_general(
                query, kconv[d, h], (((1,), (1,)), ((), ())), preferred_element_type=jnp.float32
            )
            scores.append((weights[d, h] * matched * scaling).astype(jnp.bfloat16))
        for at in range(nsp):
            for c in range(C):
                if chunks[c][0] == 1:
                    arrived(d, at, c)
                    value_copy(d, at, c).start()
        for h in range(hl):
            score = scores[h]
            denominator = jnp.sum(score.astype(jnp.float32), axis=1, keepdims=True) + fresh[d, h]
            numerator = jnp.dot(score, final[d, 1, h], preferred_element_type=jnp.float32)
            numerator = numerator + fresh[d, h] * nvalue_ref[d, h : h + 1, :].astype(jnp.float32)
            result = numerator / jnp.maximum(jnp.abs(denominator), 1.0)
            read_out[d, h : h + 1, :] = result[0:1].astype(jnp.bfloat16)

    for k in range(n):
        b = t if k == n - 1 else origin(k)
        for i in range(ns):
            for c in range(C + 1):
                if k < n - 1:
                    s1_copy(k, i, c).wait_send()
                forward(k, b, i, c, False)
    for d in range(nd):
        for at in range(nsp):
            key_copy(d, at).wait()
            for c in range(C):
                if chunks[c][0] == 1:
                    value_copy(d, at, c).wait()


def shards(
    n,
    nsp,
    layer_input,
    norm_gain,
    key_weight,
    value_weight,
    input_gate_weight,
    forget_gate_weight,
    conv_weight,
    input_shift,
    forget_shift,
    new_query,
    new_key,
    new_value,
    new_input,
    new_forget,
):
    ns, pos, width = layer_input.shape
    nd, hl, length = input_shift.shape
    dk = new_query.shape[2]
    heads = input_gate_weight.shape[1]
    taps = conv_weight.shape[0]
    dims = (n, nsp, ns, nd, pos, heads, hl, dk, taps)
    C = 2 * SPLIT
    bf16, f32 = jnp.bfloat16, jnp.float32
    vmem = pl.BlockSpec(memory_space=pltpu.VMEM)
    hbm = pl.BlockSpec(memory_space=pl.ANY)
    dma = pltpu.SemaphoreType.DMA
    return pl.pallas_call(
        functools.partial(kernel, dims),
        out_shape=(
            jax.ShapeDtypeStruct((nd, hl, length, dk), bf16),
            jax.ShapeDtypeStruct((nd, hl, length, dk), bf16),
            jax.ShapeDtypeStruct((nd, hl, length), f32),
            jax.ShapeDtypeStruct((nd, hl, dk), bf16),
        ),
        in_specs=[vmem] * 12 + [hbm] * 2,
        out_specs=(hbm, hbm, vmem, vmem),
        scratch_shapes=[
            pltpu.VMEM((n, 2, width, hl * dk), bf16),
            pltpu.VMEM((ns, pos, width), bf16),
            pltpu.VMEM((n, ns, 2, hl, pos, dk), bf16),
            pltpu.VMEM((n, ns, 2, hl, pos, dk), bf16),
            pltpu.VMEM((nd, 2, hl, length, dk), bf16),
            pltpu.VMEM((ns, 2 * heads, pos), bf16),
            pltpu.VMEM((n, ns, 2 * heads, pos), bf16),
            pltpu.VMEM((nd, nsp, 2 * heads, pos), bf16),
            pltpu.VMEM((hl, 8 + length, dk), f32),
            pltpu.VMEM((nd, hl, length, dk), bf16),
            dma((n, 2)),
            dma((n, ns, C + 1)),
            dma((n, ns, C + 1)),
            dma((n, ns, C + 1)),
            dma((nd, nsp, C + 1)),
            dma((nd, nsp, C + 1)),
        ],
        compiler_params=pltpu.CompilerParams(
            collective_id=0, has_side_effects=True, vmem_limit_bytes=60 * 1024 * 1024
        ),
    )(
        layer_input,
        norm_gain.reshape(1, width),
        input_gate_weight,
        forget_gate_weight,
        conv_weight,
        input_shift,
        forget_shift,
        new_query,
        new_key,
        new_value,
        new_input,
        new_forget,
        key_weight,
        value_weight,
    )


def solution(mesh):
    in_specs = (
        P(("grp", "tp"), "sp", None),
        P(),
        P(),
        P(),
        P(),
        P(),
        P(),
        P(("grp", "sp"), "tp", None),
        P(("grp", "sp"), "tp", None),
        P(("grp", "sp"), "tp", None),
        P(("grp", "sp"), "tp", None),
        P(("grp", "sp"), "tp", None),
        P(("grp", "sp"), "tp"),
        P(("grp", "sp"), "tp"),
    )
    out_specs = (
        P(("grp", "sp"), "tp", None, None),
        P(("grp", "sp"), "tp", None, None),
        P(("grp", "sp"), "tp", None),
        P(("grp", "sp"), "tp", None),
    )
    body = functools.partial(shards, mesh.shape["tp"], mesh.shape["sp"])
    return jax.shard_map(body, mesh=mesh, in_specs=in_specs, out_specs=out_specs, check_vma=False)
```

```python
import functools

import jax
import jax.numpy as jnp
from jax import lax
from jax.experimental import pallas as pl
from jax.experimental.pallas import tpu as pltpu
from jax.sharding import PartitionSpec as P

MESH = pl.DeviceIdType.MESH
epsilon = 1e-06
SPLIT = 2


def log_sigmoid(x):
    return jnp.minimum(x, 0.0) - jnp.log1p(jnp.exp(-jnp.abs(x)))


def kernel(
    dims,
    x_ref,
    gain_ref,
    wi_ref,
    wf_ref,
    conv_ref,
    ishift_ref,
    fshift_ref,
    query_ref,
    nkey_ref,
    nvalue_ref,
    ninput_ref,
    nforget_ref,
    wk_ref,
    wv_ref,
    keys_out,
    values_out,
    weight_out,
    read_out,
    wbuf,
    normed,
    comp,
    relay,
    final,
    gcomp,
    grelay,
    gfinal,
    ext,
    w_sem,
    s1_send,
    s1_recv,
    s2_send,
    f_recv,
):
    n, nsp, ns, nd, pos, heads, hl, dk, taps = dims
    chunks = [(kv, r) for kv in range(2) for r in range(SPLIT)]
    C = len(chunks)
    rows = pos // SPLIT
    length = nsp * pos
    t = lax.axis_index("tp")
    p = lax.axis_index("sp")
    high = (2 * t) // n
    direction = 1 - 2 * high
    targets = [lax.rem(t + direction * (1 + k) + n, n) for k in range(n)]

    barrier = pltpu.get_barrier_semaphore()
    for k in range(n - 1):
        pl.semaphore_signal(barrier, inc=1, device_id={"tp": targets[k]}, device_id_type=MESH)
    for k in range(nsp - 1):
        pl.semaphore_signal(
            barrier, inc=1, device_id={"sp": lax.rem(p + 1 + k, nsp)}, device_id_type=MESH
        )

    def weight_copy(k, kv):
        columns = pl.ds(pl.multiple_of(targets[k] * (hl * dk), dk), hl * dk)
        source = wv_ref if kv else wk_ref
        return pltpu.make_async_copy(source.at[:, columns], wbuf.at[k, kv], w_sem.at[k, kv])

    for k in range(n):
        for kv in range(2):
            weight_copy(k, kv).start()

    gain = gain_ref[...].astype(jnp.float32).reshape(1, -1)
    step = 32
    for i in range(ns):

        @pl.loop(0, pos // step)
        def _(at):
            window = pl.ds(pl.multiple_of(at * step, step), step)
            wide = x_ref[i, window, :].astype(jnp.float32)
            mean = jnp.mean(wide * wide, axis=-1, keepdims=True)
            normed[i, window, :] = (wide * lax.rsqrt(mean + epsilon) * gain).astype(jnp.bfloat16)

    def part(buf, lead, c):
        kv, r = chunks[c]
        return buf.at[(*lead, kv, slice(None), pl.ds(r * rows, rows), slice(None))]

    def s1_source(k, i, c):
        return gcomp.at[i] if c == C else part(comp, (k, i), c)

    def s1_target(b, i, c):
        return grelay.at[b, i] if c == C else part(relay, (b, i), c)

    def s1_copy(k, i, c):
        return pltpu.make_async_remote_copy(
            src_ref=s1_source(k, i, c),
            dst_ref=s1_target(t, i, c),
            send_sem=s1_send.at[k, i, c],
            recv_sem=s1_recv.at[t, i, c],
            device_id={"tp": targets[k]},
            device_id_type=MESH,
        )

    def f_target(d, at, c):
        if c == C:
            return gfinal.at[d, at]
        kv, r = chunks[c]
        window = pl.ds(pl.multiple_of(at * pos + r * rows, rows), rows)
        return (values_out if kv else final).at[d, :, window, :]

    def forward(k, b, i, c, begin):
        s = b * ns + i
        q = s // nd
        d = lax.rem(s, nd)
        source = s1_source(n - 1, i, c) if k == n - 1 else s1_target(b, i, c)
        remote = pltpu.make_async_remote_copy(
            src_ref=source,
            dst_ref=f_target(d, p, c),
            send_sem=s2_send.at[k, i, c],
            recv_sem=f_recv.at[d, p, c],
            device_id={"sp": q},
            device_id_type=MESH,
        )

        @pl.when(q != p)
        def _():
            if begin:
                remote.start()
            else:
                remote.wait_send()

        if begin:

            @pl.when(q == p)
            def _():
                pltpu.make_async_copy(source, f_target(d, p, c), f_recv.at[d, p, c]).start()

    def compute(k):
        for kv in range(2):
            weight_copy(k, kv).wait()
            for i in range(ns):
                y = jnp.dot(normed[i], wbuf[k, kv], preferred_element_type=jnp.float32)
                for h in range(hl):
                    comp[k, i, kv, h] = y[:, h * dk : (h + 1) * dk].astype(jnp.bfloat16)
            if k == 0 and kv == 0:
                pl.semaphore_wait(barrier, n - 1 + nsp - 1)
            for i in range(ns):
                for c in range(C):
                    if chunks[c][0] == kv:
                        if k == n - 1:
                            forward(k, t, i, c, True)
                        else:
                            s1_copy(k, i, c).start()

    def gates():
        for i in range(ns):
            for at, w in enumerate((wi_ref, wf_ref)):
                g = lax.dot_general(
                    w[...], normed[i], (((1,), (1,)), ((), ())), preferred_element_type=jnp.float32
                )
                gcomp[i, at * heads : (at + 1) * heads, :] = g.astype(jnp.bfloat16)
            for to in range(n - 1):
                s1_copy(to, i, C).start()
            forward(n - 1, t, i, C, True)

    for k in range(n):
        compute(k)
        if k == 0:
            gates()

    def origin(k):
        lower = k + (k >= t).astype(jnp.int32)
        upper = n - 1 - (k + (k >= n - 1 - t).astype(jnp.int32))
        return jnp.where(high == 0, lower, upper)

    def relay_step(k, c):
        b = origin(k)
        for i in range(ns):
            place = s1_target(b, i, c)
            pltpu.make_async_copy(place, place, s1_recv.at[b, i, c]).wait()
            forward(k, b, i, c, True)

    for k in range(n - 1):
        relay_step(k, C)
        for c in range(C):
            relay_step(k, c)

    def arrived(d, at, c):
        place = f_target(d, at, c)
        pltpu.make_async_copy(place, place, f_recv.at[d, at, c]).wait()

    scaling = dk ** (-0.5)
    lane = lax.broadcasted_iota(jnp.int32, (8, length), 1)
    row = lax.broadcasted_iota(jnp.int32, (2 * heads, pos), 0)
    weights, fresh = {}, {}
    for d in range(nd):
        for at in range(nsp):
            arrived(d, at, C)
        for h in range(hl):

            def gate(base):
                pieces = [
                    jnp.sum(
                        jnp.where(
                            row == base + t * hl + h, gfinal[d, at].astype(jnp.float32), 0.0
                        ),
                        axis=0,
                        keepdims=True,
                    )
                    for at in range(nsp)
                ]
                return jnp.concatenate(pieces, axis=1)

            log_forget = log_sigmoid(gate(heads) + fshift_ref[d, h : h + 1, :])
            suffix = pltpu.roll(jnp.broadcast_to(log_forget, (8, length)), length - 1, 1)
            suffix = jnp.where(lane < length - 1, suffix, 0.0)
            hop = 1
            while hop < length:
                moved = pltpu.roll(suffix, length - hop, 1)
                suffix = suffix + jnp.where(lane < length - hop, moved, 0.0)
                hop *= 2
            new_input = ninput_ref[d : d + 1, h : h + 1]
            decay = log_sigmoid(nforget_ref[d : d + 1, h : h + 1])
            log_weight = gate(0) + ishift_ref[d, h : h + 1, :] + suffix + decay
            largest = jnp.maximum(jnp.max(log_weight, axis=1, keepdims=True), new_input)
            weight = jnp.exp(log_weight - largest)
            weight_out[d, h : h + 1, :] = weight[0:1]
            query = query_ref[d, h : h + 1, :].astype(jnp.float32)
            match = jnp.sum(
                nkey_ref[d, h : h + 1, :].astype(jnp.float32) * query, axis=1, keepdims=True
            )
            score = jnp.exp(new_input - largest) * match * scaling
            fresh[d, h] = score.astype(jnp.bfloat16).astype(jnp.float32)
            weights[d, h] = weight

    for d in range(nd):
        ext[:, 0:8, :] = jnp.zeros((hl, 8, dk), jnp.float32)
        for at in range(nsp):
            for c in range(C):
                if chunks[c][0] == 0:
                    arrived(d, at, c)
            for h in range(hl):
                ext[h, 8 + at * pos : 8 + (at + 1) * pos, :] = final[
                    d, h, at * pos : (at + 1) * pos, :
                ].astype(jnp.float32)
                tap = conv_ref[
                    :, pl.ds(pl.multiple_of((t * hl + h) * dk, dk), dk)
                ]
                summed = None
                for o in range(taps):
                    start = 8 - (taps - 1) + o + at * pos
                    term = ext[h, start : start + pos, :] * tap[o : o + 1, :]
                    summed = term if summed is None else summed + term
                keys_out[d, h, at * pos : (at + 1) * pos, :] = jax.nn.silu(summed).astype(
                    jnp.bfloat16
                )
        scores = []
        for h in range(hl):
            query = jnp.broadcast_to(query_ref[d, h : h + 1, :], (8, dk))
            matched = lax.dot_general(
                query, keys_out[d, h], (((1,), (1,)), ((), ())), preferred_element_type=jnp.float32
            )
            scores.append((weights[d, h] * matched * scaling).astype(jnp.bfloat16))
        for at in range(nsp):
            for c in range(C):
                if chunks[c][0] == 1:
                    arrived(d, at, c)
        for h in range(hl):
            score = scores[h]
            denominator = jnp.sum(score.astype(jnp.float32), axis=1, keepdims=True) + fresh[d, h]
            numerator = jnp.dot(score, values_out[d, h], preferred_element_type=jnp.float32)
            numerator = numerator + fresh[d, h] * nvalue_ref[d, h : h + 1, :].astype(jnp.float32)
            result = numerator / jnp.maximum(jnp.abs(denominator), 1.0)
            read_out[d, h : h + 1, :] = result[0:1].astype(jnp.bfloat16)

    for k in range(n):
        b = t if k == n - 1 else origin(k)
        for i in range(ns):
            for c in range(C + 1):
                if k < n - 1:
                    s1_copy(k, i, c).wait_send()
                forward(k, b, i, c, False)

def write_out(*refs):
    count = (len(refs) - 1) // 2
    sem = refs[-1]
    copies = [
        pltpu.make_async_copy(refs[i], refs[count + i], sem.at[i]) for i in range(count)
    ]
    for copy in copies:
        copy.start()
    for copy in copies:
        copy.wait()


def shards(
    n,
    nsp,
    layer_input,
    norm_gain,
    key_weight,
    value_weight,
    input_gate_weight,
    forget_gate_weight,
    conv_weight,
    input_shift,
    forget_shift,
    new_query,
    new_key,
    new_value,
    new_input,
    new_forget,
):
    ns, pos, width = layer_input.shape
    nd, hl, length = input_shift.shape
    dk = new_query.shape[2]
    heads = input_gate_weight.shape[1]
    taps = conv_weight.shape[0]
    dims = (n, nsp, ns, nd, pos, heads, hl, dk, taps)
    C = 2 * SPLIT
    bf16, f32 = jnp.bfloat16, jnp.float32
    vmem = pl.BlockSpec(memory_space=pltpu.VMEM)
    hbm = pl.BlockSpec(memory_space=pltpu.HBM)
    dma = pltpu.SemaphoreType.DMA
    out_shape=(
        jax.ShapeDtypeStruct((nd, hl, length, dk), bf16),
        jax.ShapeDtypeStruct((nd, hl, length, dk), bf16),
        jax.ShapeDtypeStruct((nd, hl, length), f32),
        jax.ShapeDtypeStruct((nd, hl, dk), bf16),
    )
    held = pl.pallas_call(
        functools.partial(kernel, dims),
        out_shape=tuple(pltpu.VMEM(o.shape, o.dtype) for o in out_shape),
        in_specs=[vmem] * 12 + [hbm] * 2,
        out_specs=(vmem,) * 4,
        scratch_shapes=[
            pltpu.VMEM((n, 2, width, hl * dk), bf16),
            pltpu.VMEM((ns, pos, width), bf16),
            pltpu.VMEM((n, ns, 2, hl, pos, dk), bf16),
            pltpu.VMEM((n, ns, 2, hl, pos, dk), bf16),
            pltpu.VMEM((nd, hl, length, dk), bf16),
            pltpu.VMEM((ns, 2 * heads, pos), bf16),
            pltpu.VMEM((n, ns, 2 * heads, pos), bf16),
            pltpu.VMEM((nd, nsp, 2 * heads, pos), bf16),
            pltpu.VMEM((hl, 8 + length, dk), f32),
            dma((n, 2)),
            dma((n, ns, C + 1)),
            dma((n, ns, C + 1)),
            dma((n, ns, C + 1)),
            dma((nd, nsp, C + 1)),
        ],
        compiler_params=pltpu.CompilerParams(
            collective_id=0, has_side_effects=True, vmem_limit_bytes=60 * 1024 * 1024
        ),
    )(
        layer_input,
        norm_gain,
        input_gate_weight.T,
        forget_gate_weight.T,
        conv_weight,
        input_shift,
        forget_shift,
        new_query,
        new_key,
        new_value,
        new_input,
        new_forget,
        key_weight,
        value_weight,
    )
    return pl.pallas_call(
        write_out,
        out_shape=out_shape,
        in_specs=[vmem] * len(out_shape),
        out_specs=(hbm,) * len(out_shape),
        scratch_shapes=[dma((len(out_shape),))],
        compiler_params=pltpu.CompilerParams(vmem_limit_bytes=8 * 1024 * 1024),
    )(*held)


def solution(mesh):
    in_specs = (
        P(("grp", "tp"), "sp", None),
        P(),
        P(),
        P(),
        P(),
        P(),
        P(),
        P(("grp", "sp"), "tp", None),
        P(("grp", "sp"), "tp", None),
        P(("grp", "sp"), "tp", None),
        P(("grp", "sp"), "tp", None),
        P(("grp", "sp"), "tp", None),
        P(("grp", "sp"), "tp"),
        P(("grp", "sp"), "tp"),
    )
    out_specs = (
        P(("grp", "sp"), "tp", None, None),
        P(("grp", "sp"), "tp", None, None),
        P(("grp", "sp"), "tp", None),
        P(("grp", "sp"), "tp", None),
    )
    body = functools.partial(shards, mesh.shape["tp"], mesh.shape["sp"])
    return jax.shard_map(body, mesh=mesh, in_specs=in_specs, out_specs=out_specs, check_vma=False)
```

```python
import functools

import jax
import jax.numpy as jnp
from jax import lax
from jax.experimental import pallas as pl
from jax.experimental.pallas import tpu as pltpu
from jax.sharding import PartitionSpec as P

MESH = pl.DeviceIdType.MESH
epsilon = 1e-06
SPLIT = 2


def log_sigmoid(x):
    return jnp.minimum(x, 0.0) - jnp.log1p(jnp.exp(-jnp.abs(x)))


def kernel(
    dims,
    x_ref,
    gain_ref,
    wi_ref,
    wf_ref,
    conv_ref,
    ishift_ref,
    fshift_ref,
    query_ref,
    nkey_ref,
    nvalue_ref,
    ninput_ref,
    nforget_ref,
    wk_ref,
    wv_ref,
    keys_out,
    values_out,
    weight_out,
    read_out,
    wbuf,
    normed,
    comp,
    relay,
    final,
    gcomp,
    grelay,
    gfinal,
    ext,
    w_sem,
    s1_send,
    s1_recv,
    s2_send,
    f_recv,
):
    n, nsp, ns, nd, pos, heads, hl, dk, taps = dims
    chunks = [(kv, r) for kv in range(2) for r in range(SPLIT)]
    C = len(chunks)
    rows = pos // SPLIT
    length = nsp * pos
    t = lax.axis_index("tp")
    p = lax.axis_index("sp")
    high = (2 * t) // n
    direction = 1 - 2 * high
    targets = [lax.rem(t + direction * (1 + k) + n, n) for k in range(n)]

    barrier = pltpu.get_barrier_semaphore()
    for k in range(n - 1):
        pl.semaphore_signal(barrier, inc=1, device_id={"tp": targets[k]}, device_id_type=MESH)
    for k in range(nsp - 1):
        pl.semaphore_signal(
            barrier, inc=1, device_id={"sp": lax.rem(p + 1 + k, nsp)}, device_id_type=MESH
        )

    def weight_copy(k, kv):
        columns = pl.ds(pl.multiple_of(targets[k] * (hl * dk), dk), hl * dk)
        source = wv_ref if kv else wk_ref
        return pltpu.make_async_copy(source.at[:, columns], wbuf.at[k, kv], w_sem.at[k, kv])

    for k in range(n):
        for kv in range(2):
            weight_copy(k, kv).start()

    gain = gain_ref[...].astype(jnp.float32).reshape(1, -1)
    step = 32
    for i in range(ns):

        @pl.loop(0, pos // step)
        def _(at):
            window = pl.ds(pl.multiple_of(at * step, step), step)
            wide = x_ref[i, window, :].astype(jnp.float32)
            mean = jnp.mean(wide * wide, axis=-1, keepdims=True)
            normed[i, window, :] = (wide * lax.rsqrt(mean + epsilon) * gain).astype(jnp.bfloat16)

    def part(buf, lead, c):
        kv, r = chunks[c]
        return buf.at[(*lead, kv, slice(None), pl.ds(r * rows, rows), slice(None))]

    def s1_source(k, i, c):
        return gcomp.at[i] if c == C else part(comp, (k, i), c)

    def s1_target(b, i, c):
        return grelay.at[b, i] if c == C else part(relay, (b, i), c)

    def s1_copy(k, i, c):
        return pltpu.make_async_remote_copy(
            src_ref=s1_source(k, i, c),
            dst_ref=s1_target(t, i, c),
            send_sem=s1_send.at[k, i, c],
            recv_sem=s1_recv.at[t, i, c],
            device_id={"tp": targets[k]},
            device_id_type=MESH,
        )

    def f_target(d, at, c):
        if c == C:
            return gfinal.at[d, at]
        kv, r = chunks[c]
        window = pl.ds(pl.multiple_of(at * pos + r * rows, rows), rows)
        return (values_out if kv else final).at[d, :, window, :]

    def forward(k, b, i, c, begin):
        s = b * ns + i
        q = s // nd
        d = lax.rem(s, nd)
        source = s1_source(n - 1, i, c) if k == n - 1 else s1_target(b, i, c)
        remote = pltpu.make_async_remote_copy(
            src_ref=source,
            dst_ref=f_target(d, p, c),
            send_sem=s2_send.at[k, i, c],
            recv_sem=f_recv.at[d, p, c],
            device_id={"sp": q},
            device_id_type=MESH,
        )

        @pl.when(q != p)
        def _():
            if begin:
                remote.start()
            else:
                remote.wait_send()

        if begin:

            @pl.when(q == p)
            def _():
                pltpu.make_async_copy(source, f_target(d, p, c), f_recv.at[d, p, c]).start()

    def compute(k):
        for kv in range(2):
            weight_copy(k, kv).wait()
            for i in range(ns):
                y = jnp.dot(normed[i], wbuf[k, kv], preferred_element_type=jnp.float32)
                for h in range(hl):
                    comp[k, i, kv, h] = y[:, h * dk : (h + 1) * dk].astype(jnp.bfloat16)
            if k == 0 and kv == 0:
                pl.semaphore_wait(barrier, n - 1 + nsp - 1)
            for i in range(ns):
                for c in range(C):
                    if chunks[c][0] == kv:
                        if k == n - 1:
                            forward(k, t, i, c, True)
                        else:
                            s1_copy(k, i, c).start()

    def gates():
        for i in range(ns):
            for at, w in enumerate((wi_ref, wf_ref)):
                g = lax.dot_general(
                    w[...], normed[i], (((1,), (1,)), ((), ())), preferred_element_type=jnp.float32
                )
                gcomp[i, at * heads : (at + 1) * heads, :] = g.astype(jnp.bfloat16)
            for to in range(n - 1):
                s1_copy(to, i, C).start()
            forward(n - 1, t, i, C, True)

    for k in range(n):
        compute(k)
        if k == 0:
            gates()

    def origin(k):
        lower = k + (k >= t).astype(jnp.int32)
        upper = n - 1 - (k + (k >= n - 1 - t).astype(jnp.int32))
        return jnp.where(high == 0, lower, upper)

    def relay_step(k, c):
        b = origin(k)
        for i in range(ns):
            place = s1_target(b, i, c)
            pltpu.make_async_copy(place, place, s1_recv.at[b, i, c]).wait()
            forward(k, b, i, c, True)


    def arrived(d, at, c):
        place = f_target(d, at, c)
        pltpu.make_async_copy(place, place, f_recv.at[d, at, c]).wait()

    scaling = dk ** (-0.5)
    lane = lax.broadcasted_iota(jnp.int32, (8, length), 1)
    row = lax.broadcasted_iota(jnp.int32, (2 * heads, pos), 0)
    weights, fresh = {}, {}
    scores = {}

    def weigh():
        for d in range(nd):
            for at in range(nsp):
                arrived(d, at, C)
            for h in range(hl):

                def gate(base):
                    pieces = [
                        jnp.sum(
                            jnp.where(
                                row == base + t * hl + h, gfinal[d, at].astype(jnp.float32), 0.0
                            ),
                            axis=0,
                            keepdims=True,
                        )
                        for at in range(nsp)
                    ]
                    return jnp.concatenate(pieces, axis=1)

                log_forget = log_sigmoid(gate(heads) + fshift_ref[d, h : h + 1, :])
                suffix = pltpu.roll(jnp.broadcast_to(log_forget, (8, length)), length - 1, 1)
                suffix = jnp.where(lane < length - 1, suffix, 0.0)
                hop = 1
                while hop < length:
                    moved = pltpu.roll(suffix, length - hop, 1)
                    suffix = suffix + jnp.where(lane < length - hop, moved, 0.0)
                    hop *= 2
                new_input = ninput_ref[d : d + 1, h : h + 1]
                decay = log_sigmoid(nforget_ref[d : d + 1, h : h + 1])
                log_weight = gate(0) + ishift_ref[d, h : h + 1, :] + suffix + decay
                largest = jnp.maximum(jnp.max(log_weight, axis=1, keepdims=True), new_input)
                weight = jnp.exp(log_weight - largest)
                weight_out[d, h : h + 1, :] = weight[0:1]
                query = query_ref[d, h : h + 1, :].astype(jnp.float32)
                match = jnp.sum(
                    nkey_ref[d, h : h + 1, :].astype(jnp.float32) * query, axis=1, keepdims=True
                )
                score = jnp.exp(new_input - largest) * match * scaling
                fresh[d, h] = score.astype(jnp.bfloat16).astype(jnp.float32)
                weights[d, h] = weight


    def convolve():
        for d in range(nd):
            ext[:, 0:8, :] = jnp.zeros((hl, 8, dk), jnp.float32)
            for at in range(nsp):
                for c in range(C):
                    if chunks[c][0] == 0:
                        arrived(d, at, c)
                for h in range(hl):
                    ext[h, 8 + at * pos : 8 + (at + 1) * pos, :] = final[
                        d, h, at * pos : (at + 1) * pos, :
                    ].astype(jnp.float32)
                    tap = conv_ref[
                        :, pl.ds(pl.multiple_of((t * hl + h) * dk, dk), dk)
                    ]
                    summed = None
                    for o in range(taps):
                        start = 8 - (taps - 1) + o + at * pos
                        term = ext[h, start : start + pos, :] * tap[o : o + 1, :]
                        summed = term if summed is None else summed + term
                    keys_out[d, h, at * pos : (at + 1) * pos, :] = jax.nn.silu(summed).astype(
                        jnp.bfloat16
                    )
            for h in range(hl):
                query = jnp.broadcast_to(query_ref[d, h : h + 1, :], (8, dk))
                matched = lax.dot_general(
                    query, keys_out[d, h], (((1,), (1,)), ((), ())), preferred_element_type=jnp.float32
                )
                scores[d, h] = (weights[d, h] * matched * scaling).astype(jnp.bfloat16)

    for k in range(n - 1):
        relay_step(k, C)
    for k in range(n - 1):
        for c in range(C):
            if k == n - 2 and c == C - 1:
                if n == 2:
                    weigh()
                convolve()
            relay_step(k, c)
        if k == 0 and n > 2:
            weigh()
    if n == 1:
        weigh()
        convolve()

    for d in range(nd):
        for at in range(nsp):
            for c in range(C):
                if chunks[c][0] == 1:
                    arrived(d, at, c)
        for h in range(hl):
            score = scores[d, h]
            denominator = jnp.sum(score.astype(jnp.float32), axis=1, keepdims=True) + fresh[d, h]
            numerator = jnp.dot(score, values_out[d, h], preferred_element_type=jnp.float32)
            numerator = numerator + fresh[d, h] * nvalue_ref[d, h : h + 1, :].astype(jnp.float32)
            result = numerator / jnp.maximum(jnp.abs(denominator), 1.0)
            read_out[d, h : h + 1, :] = result[0:1].astype(jnp.bfloat16)

    for k in range(n):
        b = t if k == n - 1 else origin(k)
        for i in range(ns):
            for c in range(C + 1):
                if k < n - 1:
                    s1_copy(k, i, c).wait_send()
                forward(k, b, i, c, False)

def write_out(*refs):
    count = (len(refs) - 1) // 2
    sem = refs[-1]
    copies = [
        pltpu.make_async_copy(refs[i], refs[count + i], sem.at[i]) for i in range(count)
    ]
    for copy in copies:
        copy.start()
    for copy in copies:
        copy.wait()


def shards(
    n,
    nsp,
    layer_input,
    norm_gain,
    key_weight,
    value_weight,
    input_gate_weight,
    forget_gate_weight,
    conv_weight,
    input_shift,
    forget_shift,
    new_query,
    new_key,
    new_value,
    new_input,
    new_forget,
):
    ns, pos, width = layer_input.shape
    nd, hl, length = input_shift.shape
    dk = new_query.shape[2]
    heads = input_gate_weight.shape[1]
    taps = conv_weight.shape[0]
    dims = (n, nsp, ns, nd, pos, heads, hl, dk, taps)
    C = 2 * SPLIT
    bf16, f32 = jnp.bfloat16, jnp.float32
    vmem = pl.BlockSpec(memory_space=pltpu.VMEM)
    hbm = pl.BlockSpec(memory_space=pltpu.HBM)
    dma = pltpu.SemaphoreType.DMA
    out_shape=(
        jax.ShapeDtypeStruct((nd, hl, length, dk), bf16),
        jax.ShapeDtypeStruct((nd, hl, length, dk), bf16),
        jax.ShapeDtypeStruct((nd, hl, length), f32),
        jax.ShapeDtypeStruct((nd, hl, dk), bf16),
    )
    held = pl.pallas_call(
        functools.partial(kernel, dims),
        out_shape=tuple(pltpu.VMEM(o.shape, o.dtype) for o in out_shape),
        in_specs=[vmem] * 12 + [hbm] * 2,
        out_specs=(vmem,) * 4,
        scratch_shapes=[
            pltpu.VMEM((n, 2, width, hl * dk), bf16),
            pltpu.VMEM((ns, pos, width), bf16),
            pltpu.VMEM((n, ns, 2, hl, pos, dk), bf16),
            pltpu.VMEM((n, ns, 2, hl, pos, dk), bf16),
            pltpu.VMEM((nd, hl, length, dk), bf16),
            pltpu.VMEM((ns, 2 * heads, pos), bf16),
            pltpu.VMEM((n, ns, 2 * heads, pos), bf16),
            pltpu.VMEM((nd, nsp, 2 * heads, pos), bf16),
            pltpu.VMEM((hl, 8 + length, dk), f32),
            dma((n, 2)),
            dma((n, ns, C + 1)),
            dma((n, ns, C + 1)),
            dma((n, ns, C + 1)),
            dma((nd, nsp, C + 1)),
        ],
        compiler_params=pltpu.CompilerParams(
            collective_id=0, has_side_effects=True, vmem_limit_bytes=60 * 1024 * 1024
        ),
    )(
        layer_input,
        norm_gain,
        input_gate_weight.T,
        forget_gate_weight.T,
        conv_weight,
        input_shift,
        forget_shift,
        new_query,
        new_key,
        new_value,
        new_input,
        new_forget,
        key_weight,
        value_weight,
    )
    return pl.pallas_call(
        write_out,
        out_shape=out_shape,
        in_specs=[vmem] * len(out_shape),
        out_specs=(hbm,) * len(out_shape),
        scratch_shapes=[dma((len(out_shape),))],
        compiler_params=pltpu.CompilerParams(vmem_limit_bytes=8 * 1024 * 1024),
    )(*held)


def solution(mesh):
    in_specs = (
        P(("grp", "tp"), "sp", None),
        P(),
        P(),
        P(),
        P(),
        P(),
        P(),
        P(("grp", "sp"), "tp", None),
        P(("grp", "sp"), "tp", None),
        P(("grp", "sp"), "tp", None),
        P(("grp", "sp"), "tp", None),
        P(("grp", "sp"), "tp", None),
        P(("grp", "sp"), "tp"),
        P(("grp", "sp"), "tp"),
    )
    out_specs = (
        P(("grp", "sp"), "tp", None, None),
        P(("grp", "sp"), "tp", None, None),
        P(("grp", "sp"), "tp", None),
        P(("grp", "sp"), "tp", None),
    )
    body = functools.partial(shards, mesh.shape["tp"], mesh.shape["sp"])
    return jax.shard_map(body, mesh=mesh, in_specs=in_specs, out_specs=out_specs, check_vma=False)
```
